32 devices in a mesh: sp: 8 (over z, y), tp: 4 (over x, core).
Axes of the slice: x: 2, y: 2, z: 4, core: 2. Of those that a mesh axis runs over, the one named last changes fastest.
Arguments:
- tokens: bfloat16 [8192, 2048], P('sp'), may hold values from -6 to 6
- norm_gain: float32 [2048], replicated, may hold values from 0.1 to 1.9
- q_down: bfloat16 [2048, 768], replicated, may hold values from -0.125 to 0.125
- kv_down: bfloat16 [2048, 512], replicated, may hold values from -0.125 to 0.125
- rope_down: bfloat16 [2048, 32], replicated, may hold values from -0.125 to 0.125
- q_latent_gain: float32 [768], replicated, may hold values from 0.1 to 1.9
- kv_latent_gain: float32 [512], replicated, may hold values from 0.1 to 1.9
- q_up: bfloat16 [768, 1536], P(None, 'tp'), may hold values from -6 to 6
- kv_up: bfloat16 [512, 2048], P(None, 'tp'), may hold values from -0.25 to 0.25
- window_query: bfloat16 [2048, 1024], P(None, 'tp'), may hold values from -6 to 6
- window_key: bfloat16 [2048, 512], P(None, 'tp'), may hold values from -0.125 to 0.125
- window_value: bfloat16 [2048, 512], P(None, 'tp'), may hold values from -0.125 to 0.125
- sink_logit: float32 [16], P('tp'), may hold values from 2 to 6
- gate_latent: bfloat16 [2048, 2048], P(None, 'tp'), may hold values from -0.125 to 0.125
- gate_window: bfloat16 [2048, 2048], P(None, 'tp'), may hold values from -0.125 to 0.125
- latent_out: bfloat16 [1024, 2048], P(None, 'tp'), may hold values from -0.1875 to 0.1875
- window_out: bfloat16 [1024, 2048], P(None, 'tp'), may hold values from -0.1875 to 0.1875
- out_gain: float32 [2048], P('tp'), may hold values from 0.1 to 1.9
Outputs:
- mixed: bfloat16 [8192, 2048], P('sp', 'tp')
The draws below stay inside these ranges and needn't reach their ends.
All inputs are finite; a program needn't handle non-finite values.
Results may differ from the reference program's by a relative error of at most 0.014.
The reference program's roundings to bfloat16 on the way count: a program that leaves them out, or rounds other values in their place, can miss the bound.
Values may be sent and summed in bfloat16 or wider, within the bound.
A program may use at most 128 MiB of HBM per device.

```python
import math
import jax
import jax.numpy as jnp
from jax import lax

D = 2048
AH = 16
NOPE = 64
ROPE = 32
VDIM = 64
QR = 768
KVR = 512
CH = 16
CKV = 8
CDH = 64
WINDOW = 128
TOKENS = 8192


def head_scaled(key, row_count, head_count, head_width):
    sample_values = jax.random.normal(jax.random.fold_in(key, 11), (row_count, head_count, head_width), jnp.float32) * row_count ** (-0.5)
    return jnp.clip(sample_values, -6.0, 6.0).reshape(row_count, head_count * head_width)


def draw_q_up(key, part):
    return head_scaled(key, QR, AH, NOPE + ROPE).astype(jnp.bfloat16)


def draw_window_query(key, part):
    return head_scaled(key, D, CH, CDH).astype(jnp.bfloat16)


def shard_levels(rng, shape, split, least, largest):
    loudness = 1.0
    for axis_at, blocks in split:
        steps = jax.random.uniform(jax.random.fold_in(jax.random.fold_in(rng, 6), axis_at), (blocks,), jnp.float32, least / len(split), largest / len(split))
        loudness = loudness * jnp.repeat(jnp.exp(steps), shape[axis_at] // blocks).reshape((-1,) + (1,) * (len(shape) - 1 - axis_at))
    return loudness


def scatter_about(rng, extent, deviation, reach, split=(), kind=jnp.bfloat16):
    entries = deviation * jax.random.normal(rng, extent, jnp.float32)
    if split:
        entries = entries * shard_levels(rng, extent, split, -0.22, 0.18)
    return jnp.clip(entries, -reach, reach).astype(kind)


def setup_inputs(seed: int = 0) -> dict:
    key_of = jax.random.split(jax.random.key(seed), 19)
    return {
        "tokens": scatter_about(key_of[0], (TOKENS, D), 1.0, 6.0, ((0, 8),)),
        "norm_gain": jnp.clip(1.0 + 0.18 * jax.random.normal(key_of[1], (D,), jnp.float32), 0.1, 1.9),
        "q_down": scatter_about(key_of[2], (D, QR), D ** -0.5, 0.125),
        "kv_down": scatter_about(key_of[3], (D, KVR), D ** -0.5, 0.125),
        "rope_down": scatter_about(key_of[4], (D, ROPE), D ** -0.5, 0.125),
        "q_latent_gain": jnp.clip(1.0 + 0.18 * jax.random.normal(key_of[5], (QR,), jnp.float32), 0.1, 1.9),
        "kv_latent_gain": jnp.clip(1.0 + 0.18 * jax.random.normal(key_of[6], (KVR,), jnp.float32), 0.1, 1.9),
        "q_up": draw_q_up(jax.random.fold_in(key_of[18], 71), 0),
        "kv_up": scatter_about(key_of[8], (KVR, AH * (NOPE + VDIM)), KVR ** -0.5, 0.25, ((1, 4),)),
        "window_query": draw_window_query(jax.random.fold_in(key_of[18], 71), 0),
        "window_key": scatter_about(key_of[10], (D, CKV * CDH), D ** -0.5, 0.125, ((1, 4),)),
        "window_value": scatter_about(key_of[11], (D, CKV * CDH), D ** -0.5, 0.125, ((1, 4),)),
        "sink_logit": jnp.clip(2.0 + 4.0 * jax.random.uniform(key_of[12], (CH,), jnp.float32) ** shard_levels(key_of[12], (CH,), ((0, 4),), -0.2, 0.2), 2.0, 6.0),
        "gate_latent": scatter_about(key_of[13], (D, D), D ** -0.5, 0.125, ((1, 4),)),
        "gate_window": scatter_about(key_of[14], (D, D), D ** -0.5, 0.125, ((1, 4),)),
        "latent_out": scatter_about(key_of[15], (AH * VDIM, D), (AH * VDIM) ** -0.5, 0.1875, ((1, 4),)),
        "window_out": scatter_about(key_of[16], (CH * CDH, D), (CH * CDH) ** -0.5, 0.1875, ((1, 4),)),
        "out_gain": jnp.clip(1.0 + 0.18 * jax.random.normal(key_of[17], (D,), jnp.float32), 0.1, 1.9),
    }


eps = 1e-06

def rms_scale(values, gain):
    return values * lax.rsqrt(lax.optimization_barrier(jnp.mean(values * values, axis=-1, keepdims=True)) + eps) * gain

def rotate(values, positions):
    half_width = values.shape[-1] // 2
    inverse = 10000.0 ** (-jnp.arange(half_width, dtype=jnp.float32) / half_width)
    angles = positions.astype(jnp.float32)[:, None] * inverse[None, :]
    cosine = jnp.cos(angles)[:, None, :]
    sine_val = jnp.sin(angles)[:, None, :]
    first_half = values[..., :half_width]
    second_half = values[..., half_width:]
    return jnp.concatenate([first_half * cosine - second_half * sine_val, first_half * sine_val + second_half * cosine], axis=-1)

def reference(tokens, norm_gain, q_down, kv_down, rope_down, q_latent_gain, kv_latent_gain, q_up, kv_up, window_query, window_key, window_value, sink_logit, gate_latent, gate_window, latent_out, window_out, out_gain):
    seq_len = tokens.shape[0]
    positions = jnp.arange(seq_len, dtype=jnp.int32)
    normed = rms_scale(tokens.astype(jnp.float32), norm_gain).astype(jnp.bfloat16)
    q_lat = rms_scale(jnp.dot(normed, q_down, preferred_element_type=jnp.float32), q_latent_gain).astype(jnp.bfloat16)
    kv_lat = rms_scale(jnp.dot(normed, kv_down, preferred_element_type=jnp.float32), kv_latent_gain).astype(jnp.bfloat16)
    rope_key = rotate(jnp.dot(normed, rope_down, preferred_element_type=jnp.float32)[:, None, :], positions)[:, 0, :].astype(jnp.bfloat16)
    queries = jnp.dot(q_lat, q_up, preferred_element_type=jnp.float32).reshape(seq_len, AH, NOPE + ROPE)
    queries = jnp.concatenate([queries[..., :NOPE], rotate(queries[..., NOPE:], positions)], axis=-1).astype(jnp.bfloat16)
    keyval = jnp.dot(kv_lat, kv_up, preferred_element_type=jnp.float32).astype(jnp.bfloat16).reshape(seq_len, AH, NOPE + VDIM)
    key_nope = keyval[..., :NOPE].astype(jnp.float32)
    latent_values = keyval[..., NOPE:].astype(jnp.float32)
    rope_wide = rope_key.astype(jnp.float32)
    score_scale = (NOPE + ROPE) ** (-0.5)
    block_rows = math.gcd(seq_len, 256)

    def latent_block(q_block):
        q_wide = q_block.astype(jnp.float32)
        scores = (jnp.einsum('qhd,khd->qhk', q_wide[..., :NOPE], key_nope) + jnp.einsum('qhd,kd->qhk', q_wide[..., NOPE:], rope_wide)) * score_scale
        top_score = lax.optimization_barrier(jnp.max(scores, axis=-1, keepdims=True))
        weights = jnp.exp(scores - top_score)
        weight_sum = lax.optimization_barrier(jnp.sum(weights, axis=-1))
        rounded = lax.optimization_barrier(weights.astype(jnp.bfloat16)).astype(jnp.float32)
        summed = jnp.einsum('qhk,khd->qhd', rounded, latent_values)
        return (summed / weight_sum[..., None]).astype(jnp.bfloat16).reshape(q_block.shape[0], AH * VDIM)
    latent_heads = lax.map(latent_block, queries.reshape(seq_len // block_rows, block_rows, AH, NOPE + ROPE)).reshape(seq_len, AH * VDIM)
    group_size = CH // CKV
    window_q = jnp.dot(normed, window_query, preferred_element_type=jnp.float32).astype(jnp.bfloat16).reshape(seq_len, CKV, group_size, CDH)
    window_k = jnp.dot(normed, window_key, preferred_element_type=jnp.float32).astype(jnp.bfloat16).reshape(seq_len, CKV, CDH)
    window_v = jnp.dot(normed, window_value, preferred_element_type=jnp.float32).astype(jnp.bfloat16).reshape(seq_len, CKV, CDH)
    padding = ((WINDOW, WINDOW), (0, 0), (0, 0))
    keys_pad = jnp.pad(window_k, padding)
    values_pad = jnp.pad(window_v, padding)
    span_rows = math.gcd(seq_len, 512)
    span_len = span_rows + 2 * WINDOW
    sink_rows = sink_logit.reshape(CKV, group_size)[:, :, None]

    def window_block(block_index):
        first_row = block_index * span_rows
        q_block = lax.dynamic_slice_in_dim(window_q, first_row, span_rows, 0).astype(jnp.float32)
        k_block = lax.dynamic_slice_in_dim(keys_pad, first_row, span_len, 0).astype(jnp.float32)
        v_block = lax.dynamic_slice_in_dim(values_pad, first_row, span_len, 0).astype(jnp.float32)
        scores = jnp.einsum('qkgd,skd->kgqs', q_block, k_block) * CDH ** (-0.5)
        offsets = jnp.arange(span_len, dtype=jnp.int32)[None, :] - WINDOW - jnp.arange(span_rows, dtype=jnp.int32)[:, None]
        key_pos = first_row - WINDOW + jnp.arange(span_len, dtype=jnp.int32)
        allowed = (jnp.abs(offsets) <= WINDOW) & ((key_pos >= 0) & (key_pos < seq_len))[None, :]
        scores = jnp.where(allowed, scores, -1e+30)
        top_score = jnp.maximum(lax.optimization_barrier(jnp.max(scores, axis=-1)), sink_rows)
        weights = jnp.where(allowed, jnp.exp(scores - top_score[..., None]), 0.0)
        normalizer = lax.optimization_barrier(jnp.sum(weights, axis=-1)) + jnp.exp(sink_rows - top_score)
        rounded = lax.optimization_barrier(weights.astype(jnp.bfloat16)).astype(jnp.float32)
        summed = jnp.einsum('kgqs,skd->qkgd', rounded, v_block)
        return (summed / jnp.moveaxis(normalizer, -1, 0)[..., None]).astype(jnp.bfloat16).reshape(span_rows, CH * CDH)
    window_heads = lax.map(window_block, jnp.arange(seq_len // span_rows, dtype=jnp.int32)).reshape(seq_len, CH * CDH)
    proj_latent = jnp.dot(latent_heads, latent_out, preferred_element_type=jnp.float32)
    proj_window = jnp.dot(window_heads, window_out, preferred_element_type=jnp.float32)
    merged = jax.nn.sigmoid(jnp.dot(normed, gate_latent, preferred_element_type=jnp.float32)) * proj_latent + jax.nn.sigmoid(jnp.dot(normed, gate_window, preferred_element_type=jnp.float32)) * proj_window
    return rms_scale(merged, out_gain).astype(jnp.bfloat16)
```

```python
import functools
import math

import jax
import jax.numpy as jnp
from jax import lax
from jax.experimental import pallas as pl
from jax.experimental.pallas import tpu as pltpu
from jax.sharding import PartitionSpec as P

D = 2048
NOPE = 64
ROPE = 32
VDIM = 64
QR = 768
CH = 16
CKV = 8
CDH = 64
WINDOW = 128


eps = 1e-06


def padded_2(shard, sides, width):
    for axis, dim in sides:
        size, length = (lax.axis_size(axis), shard.shape[dim])
        up = [(i, (i + 1) % size) for i in range(size - 1)]
        down = [(j, i) for i, j in up]
        last = lax.slice_in_dim(shard, length - width, length, axis=dim)
        first = lax.slice_in_dim(shard, 0, width, axis=dim)
        before = lax.ppermute(last, axis, up)
        after = lax.ppermute(first, axis, down)
        shard = jnp.concatenate([before, shard, after], axis=dim)
    return shard


def rms_scale(values, gain):
    return values * lax.rsqrt(jnp.mean(values * values, axis=-1, keepdims=True) + eps) * gain


def rotate(values, positions):
    half_width = values.shape[-1] // 2
    inverse = 10000.0 ** (-jnp.arange(half_width, dtype=jnp.float32) / half_width)
    angles = positions.astype(jnp.float32)[:, None] * inverse[None, :]
    cosine = jnp.cos(angles)[:, None, :]
    sine_val = jnp.sin(angles)[:, None, :]
    first_half = values[..., :half_width]
    second_half = values[..., half_width:]
    return jnp.concatenate(
        [
            first_half * cosine - second_half * sine_val,
            first_half * sine_val + second_half * cosine,
        ],
        axis=-1,
    )


LANES = 128
LOG2E = 1.4426950408889634
Q_TILE = 256
KEY_TILE = 2048


def latent_kernel(pair, scale, q_ref, key_ref, rope_ref, value_ref, out_ref, keys, q_shift, acc, top):
    rows, key_count = (q_ref.shape[0], keys.shape[1])
    q_tile = math.gcd(rows, Q_TILE)
    key_tile = math.gcd(key_count, KEY_TILE)
    head_dim = NOPE + ROPE
    keys[:NOPE, :] = key_ref[...]
    keys[NOPE:head_dim, :] = rope_ref[...]
    tail = lax.broadcasted_iota(jnp.int32, (LANES - head_dim, key_count), 0)
    keys[head_dim:, :] = jnp.where(tail == 0, 1.0, 0.0).astype(jnp.bfloat16)
    ones_lane = jnp.where(
        lax.broadcasted_iota(jnp.int32, (1, LANES), 1) == VDIM, 1.0, 0.0
    ).astype(jnp.bfloat16)
    lane = lax.broadcasted_iota(jnp.int32, (q_tile, LANES), 1)
    for first in range(0, rows, q_tile):
        part = q_ref[first : first + q_tile, :]
        scores = jnp.dot(part, keys[:, :256], preferred_element_type=jnp.float32)
        shift = jnp.max(scores, axis=-1, keepdims=True)
        q_shift[first : first + q_tile, :] = jnp.where(
            lane == head_dim, -shift, part.astype(jnp.float32)
        ).astype(jnp.bfloat16)

    acc[...] = jnp.zeros_like(acc)

    def key_step(step, carry):
        span = pl.ds(pl.multiple_of(step * key_tile, key_tile), key_tile)
        key_block = keys[:, span]
        value_block = value_ref[span, :] + ones_lane
        for first in range(0, rows, q_tile):
            at = slice(first, first + q_tile)
            scores = jnp.dot(q_shift[at, :], key_block, preferred_element_type=jnp.float32)
            weights = jnp.exp2(scores * scale).astype(jnp.bfloat16)
            acc[at, :] += jnp.dot(weights, value_block, preferred_element_type=jnp.float32)
        return carry

    lax.fori_loop(0, key_count // key_tile, key_step, 0)
    sums = acc[:, VDIM : VDIM + 1]
    unsafe = jnp.max(jnp.where((sums > 1e-30) & (sums < 1e30), 0.0, 1.0)) > 0.5

    @pl.when(unsafe)
    def _():
        acc[...] = jnp.zeros_like(acc)
        top[...] = jnp.full_like(top, -1e30)

        def careful_step(step, carry):
            row_at = step // (key_count // 256)
            at = pl.ds(pl.multiple_of(row_at * q_tile, q_tile), q_tile)
            span = pl.ds(pl.multiple_of((step % (key_count // 256)) * 256, 256), 256)
            scores = jnp.dot(q_shift[at, :], keys[:, span], preferred_element_type=jnp.float32)
            old_top = top[at, :1]
            new_top = jnp.maximum(old_top, jnp.max(scores, axis=-1, keepdims=True))
            weights = jnp.exp2((scores - new_top) * scale).astype(jnp.bfloat16)
            acc[at, :] = acc[at, :] * jnp.exp2((old_top - new_top) * scale) + jnp.dot(
                weights, value_ref[span, :] + ones_lane, preferred_element_type=jnp.float32
            )
            top[at, :] = jnp.broadcast_to(new_top, (q_tile, LANES))
            return carry

        lax.fori_loop(0, (rows // q_tile) * (key_count // 256), careful_step, 0)

    result = (acc[:, :VDIM] / acc[:, VDIM : VDIM + 1]).astype(jnp.bfloat16)
    for slot in range(pair):

        @pl.when(pl.program_id(0) % pair == slot)
        def _():
            out_ref[:, slot * VDIM : (slot + 1) * VDIM] = result


def latent_attention(queries, keys_t, rope_t, values, first_head, head_count):
    rows = queries.shape[0]
    key_count = keys_t.shape[1]
    pair = 2 if head_count % 2 == 0 else 1
    assert pair == 2 or head_count == 1
    work = head_count * rows * key_count
    return pl.pallas_call(
        functools.partial(latent_kernel, pair, LOG2E * (NOPE + ROPE) ** (-0.5)),
        grid=(head_count,),
        in_specs=[
            pl.BlockSpec((rows, LANES), lambda h: (0, first_head + h)),
            pl.BlockSpec((NOPE, key_count), lambda h: (first_head + h, 0)),
            pl.BlockSpec((ROPE, key_count), lambda h: (0, 0)),
            pl.BlockSpec((key_count, LANES), lambda h: (0, first_head + h)),
        ],
        out_specs=pl.BlockSpec((rows, pair * VDIM), lambda h: (0, h // pair)),
        out_shape=jax.ShapeDtypeStruct((rows, head_count * VDIM), jnp.bfloat16),
        scratch_shapes=[
            pltpu.VMEM((LANES, key_count), jnp.bfloat16),
            pltpu.VMEM((rows, LANES), jnp.bfloat16),
            pltpu.VMEM((rows, LANES), jnp.float32),
            pltpu.VMEM((rows, LANES), jnp.float32),
        ],
        compiler_params=pltpu.CompilerParams(vmem_limit_bytes=48 * 1024 * 1024),
        cost_estimate=pl.CostEstimate(
            flops=2 * work * 512, bytes_accessed=head_count * key_count * 512, transcendentals=work
        ),
    )(queries, keys_t, rope_t, values)


def shards(
    tokens,
    norm_gain,
    q_down,
    kv_down,
    rope_down,
    q_latent_gain,
    kv_latent_gain,
    q_up,
    kv_up,
    window_query,
    window_key,
    window_value,
    sink_logit,
    gate_latent,
    gate_window,
    latent_out,
    window_out,
    out_gain,
):
    tok_rows = tokens.shape[0]
    tp_count = lax.axis_size("tp")
    seq_offset = lax.axis_index("sp") * tok_rows
    seq_len = tok_rows * lax.axis_size("sp")
    slice_rows = tok_rows // tp_count
    slice_first = lax.axis_index("tp") * slice_rows
    normed = rms_scale(tokens.astype(jnp.float32), norm_gain).astype(jnp.bfloat16)
    positions = seq_offset + jnp.arange(tok_rows, dtype=jnp.int32)
    rope_key = rotate(
        jnp.dot(normed, rope_down, preferred_element_type=jnp.float32)[:, None, :], positions
    )[:, 0, :].astype(jnp.bfloat16)
    head_dim = NOPE + ROPE
    heads_here = q_up.shape[1] // head_dim
    q_lat = rms_scale(
        jnp.dot(normed, q_down, preferred_element_type=jnp.float32), q_latent_gain
    ).astype(jnp.bfloat16)
    kv_every = rms_scale(
        jnp.dot(normed, kv_down, preferred_element_type=jnp.float32), kv_latent_gain
    ).astype(jnp.bfloat16)
    shard_rows = jnp.concatenate([q_lat, kv_every], axis=1)
    row_count = shard_rows.shape[0]
    row_pos = seq_offset + jnp.arange(row_count, dtype=jnp.int32)
    queries = jnp.dot(shard_rows[:, :QR], q_up, preferred_element_type=jnp.float32).reshape(
        row_count, heads_here, head_dim
    )
    queries = jnp.concatenate([queries[..., :NOPE], rotate(queries[..., NOPE:], row_pos)], axis=-1)
    queries = queries.astype(jnp.bfloat16)
    queries = jnp.pad(queries, ((0, 0), (0, 0), (0, LANES - head_dim))).reshape(
        row_count, heads_here * LANES
    )
    own_rows = lax.dynamic_slice_in_dim(
        jnp.concatenate([kv_every, rope_key], axis=1), slice_first, slice_rows, 0
    )
    every_row = lax.all_gather(own_rows, ("sp", "tp"), axis=0, tiled=True)
    gated = [
        jax.nn.sigmoid(jnp.dot(normed, gate, preferred_element_type=jnp.float32))
        for gate in (gate_latent, gate_window)
    ]
    every_row, *gated = lax.optimization_barrier((every_row, *gated))
    kv_rank = kv_every.shape[1]
    lat_rows = every_row[:, :kv_rank]
    rope_t = every_row[:, kv_rank:].T
    up_heads = kv_up.reshape(kv_rank, heads_here, NOPE + VDIM)
    key_up = up_heads[:, :, :NOPE].reshape(kv_rank, heads_here * NOPE)
    value_up = jnp.pad(up_heads[:, :, NOPE:], ((0, 0), (0, 0), (0, LANES - VDIM))).reshape(
        kv_rank, heads_here * LANES
    )
    keys_t = lax.dot_general(
        key_up, lat_rows, (((0,), (1,)), ((), ())), preferred_element_type=jnp.float32
    ).astype(jnp.bfloat16)
    values = jnp.dot(lat_rows, value_up, preferred_element_type=jnp.float32).astype(jnp.bfloat16)
    groups = 2 if heads_here % 2 == 0 else 1
    group_heads = heads_here // groups
    latent_pieces = []
    for group in range(groups):
        heads = latent_attention(
            queries, keys_t, rope_t, values, group * group_heads, group_heads
        )
        latent_pieces.append(lax.all_gather(heads, "tp", axis=1, tiled=True))
    kv_here = window_key.shape[1] // CDH
    group_size = CH // CKV
    window_q = (
        jnp.dot(normed, window_query, preferred_element_type=jnp.float32)
        .astype(jnp.bfloat16)
        .reshape(tok_rows, kv_here, group_size, CDH)
    )
    key_value = jnp.concatenate(
        [
            jnp.dot(normed, window_key, preferred_element_type=jnp.float32).astype(jnp.bfloat16),
            jnp.dot(normed, window_value, preferred_element_type=jnp.float32).astype(jnp.bfloat16),
        ],
        axis=1,
    )
    padded = padded_2(key_value, (("sp", 0),), WINDOW)
    span_rows = math.gcd(tok_rows, 512)
    span_len = span_rows + 2 * WINDOW
    sink_rows = sink_logit.reshape(kv_here, group_size)[:, :, None]

    def window_block(block_index):
        first_row = block_index * span_rows
        q_block = lax.dynamic_slice_in_dim(window_q, first_row, span_rows, 0)
        key_block = lax.dynamic_slice_in_dim(padded, first_row, span_len, 0)
        key_rows = key_block[:, : kv_here * CDH].reshape(span_len, kv_here, CDH)
        value_rows = key_block[:, kv_here * CDH :].reshape(span_len, kv_here, CDH)
        scores = jnp.einsum(
            "qkgd,skd->kgqs", q_block, key_rows, preferred_element_type=jnp.float32
        ) * CDH ** (-0.5)
        offsets = (
            jnp.arange(span_len, dtype=jnp.int32)[None, :]
            - WINDOW
            - jnp.arange(span_rows, dtype=jnp.int32)[:, None]
        )
        key_pos = seq_offset + first_row - WINDOW + jnp.arange(span_len, dtype=jnp.int32)
        allowed = (jnp.abs(offsets) <= WINDOW) & ((key_pos >= 0) & (key_pos < seq_len))[None, :]
        scores = jnp.where(allowed, scores, -1e30)
        top_score = jnp.maximum(jnp.max(scores, axis=-1), sink_rows)
        weights = jnp.where(allowed, jnp.exp(scores - top_score[..., None]), 0.0)
        normalizer = jnp.sum(weights, axis=-1) + jnp.exp(sink_rows - top_score)
        summed = jnp.einsum(
            "kgqs,skd->qkgd",
            weights.astype(jnp.bfloat16),
            value_rows,
            preferred_element_type=jnp.float32,
        )
        result = summed / jnp.moveaxis(normalizer, -1, 0)[..., None]
        return result.astype(jnp.bfloat16).reshape(span_rows, kv_here * group_size * CDH)

    window_heads = lax.map(
        window_block, jnp.arange(tok_rows // span_rows, dtype=jnp.int32)
    ).reshape(tok_rows, kv_here * group_size * CDH)
    window_part = lax.all_gather(window_heads, "tp", axis=1, tiled=True)
    out_width = latent_out.shape[1]
    out_rows = latent_out.reshape(tp_count, groups, group_heads * VDIM, out_width)
    proj_latent = sum(
        jnp.dot(
            piece,
            out_rows[:, group].reshape(piece.shape[1], out_width),
            preferred_element_type=jnp.float32,
        )
        for group, piece in enumerate(latent_pieces)
    )
    proj_window = jnp.dot(window_part, window_out, preferred_element_type=jnp.float32)
    merged = gated[0] * proj_latent + gated[1] * proj_window
    squares = lax.psum(jnp.sum(merged * merged, axis=1), "tp")
    mixed_out = merged * lax.rsqrt(squares / D + eps)[:, None] * out_gain
    return mixed_out.astype(jnp.bfloat16)


def solution(mesh):
    placed = (
        P("sp", None),
        P(),
        P(),
        P(),
        P(),
        P(),
        P(),
        P(None, "tp"),
        P(None, "tp"),
        P(None, "tp"),
        P(None, "tp"),
        P(None, "tp"),
        P("tp"),
        P(None, "tp"),
        P(None, "tp"),
        P(None, "tp"),
        P(None, "tp"),
        P("tp"),
    )
    return jax.shard_map(
        shards, mesh=mesh, in_specs=placed, out_specs=P("sp", "tp"), check_vma=False
    )
```
